32 devices in a mesh: grp: 2 (over x), ep: 16 (over z, y, core).
Axes of the slice: x: 2, y: 2, z: 4, core: 2. Of those that a mesh axis runs over, the one named last changes fastest.
Arguments:
- tokens: bfloat16 [1024, 2048], P(('grp', 'ep')), parts along dimension 0, may hold values from -6 to 6
- routing: int32 [1024, 4], P(('grp', 'ep')), parts along dimension 0, may hold values from 0 to 15, as said below
- gate_weights: float32 [1024, 4], P(('grp', 'ep')), parts along dimension 0, may hold values from 0.05 to 1
- pre_gain: float32 [2048], replicated, may hold values from 0.1 to 1.9
- w_gate: bfloat16 [16, 2048, 512], P('ep'), may hold values from -0.125 to 0.125
- w_up: bfloat16 [16, 2048, 512], P('ep'), may hold values from -0.125 to 0.125
- w_down: bfloat16 [16, 512, 2048], P('ep'), may hold values from -0.25 to 0.25
- post_gain: float32 [2048], replicated, may hold values from 0.1 to 1.9
Outputs:
- mixed_out: bfloat16 [1024, 2048], P(('grp', 'ep')), parts along dimension 0
The draws below stay inside these ranges and needn't reach their ends.
There are 2 independent parts, one for each index of `grp`. The reference program is written for one: setup_inputs(seed, part) draws one part's arguments, and reference() takes and returns one part's arrays. A program takes and returns all parts, laid end to end along the dimension named above; an argument that names none is the same for every part. Nothing has to cross between parts.
Inputs may be any that keep to these rules, and one draw needn't show every extreme that they name: `routing`: each row names 4 different experts of one group (experts g * 8 to g * 8 + 7). The rows of one device name any one expert at most 16 times, and some expert exactly 16 times.
All inputs are finite; a program needn't handle non-finite values.
Results may differ from the reference program's by a relative error of at most 0.0085.
Values may be sent and summed in bfloat16 or wider, within the bound.
A program may use at most 64 MiB of HBM per device.

```python
import math
import jax
import jax.numpy as jnp
from jax import lax

D = 2048
EXPERT_FF = 512
TOPK = 4
EXP_GROUP = 8
TOK_DEV = 32
EXPERTS = 16
SPECIALIST_SETS = 2
CAP = 16
TOKENS = 512
N_EP = 16


def draw_routing(key, part):
    group_slots = 2 * CAP
    slot_count = SPECIALIST_SETS * group_slots
    sampler_seeds = jax.random.split(key, 5)
    affinity_increment = jax.random.permutation(sampler_seeds[0], SPECIALIST_SETS).astype(jnp.int32) * (1024 // SPECIALIST_SETS)
    mandated_cluster = jax.random.randint(sampler_seeds[1], (N_EP,), 0, SPECIALIST_SETS)
    affinity_jitter = jax.random.randint(sampler_seeds[2], (N_EP, slot_count), 0, 1024)
    slot_ids = jnp.arange(slot_count, dtype=jnp.int32)
    cluster_for_position = slot_ids // group_slots
    cluster_affinity = affinity_jitter + affinity_increment[cluster_for_position][None, :] + jnp.where(cluster_for_position[None, :] == mandated_cluster[:, None], 4096, 0)
    cluster_affinity = cluster_affinity * slot_count + slot_ids[None, :]
    chosen = lax.top_k(cluster_affinity, TOK_DEV)[1].astype(jnp.int32)
    shuffle = jax.random.randint(sampler_seeds[3], (N_EP, TOK_DEV), 0, 1 << 20) * TOK_DEV + jnp.arange(TOK_DEV, dtype=jnp.int32)[None, :]
    chosen = jnp.take_along_axis(chosen, jnp.argsort(shuffle, axis=1, stable=True), axis=1)
    group_of = chosen // group_slots
    rank_of = chosen % group_slots
    offsets = jax.random.randint(sampler_seeds[4], (N_EP, SPECIALIST_SETS), 0, EXP_GROUP)
    offset_of = jnp.take_along_axis(offsets, group_of, axis=1)
    within = (offset_of[..., None] + rank_of[..., None] * TOPK + jnp.arange(TOPK, dtype=jnp.int32)) % EXP_GROUP
    return (group_of[..., None] * EXP_GROUP + within).reshape(TOKENS, TOPK).astype(jnp.int32)


def levels(stream_key, shape, cuts, low, largest):
    factor_of, own = 1.0, jax.random.fold_in(stream_key, 6)
    for axis_at, shards_of in cuts:
        heights = jnp.exp(jax.random.uniform(jax.random.fold_in(own, axis_at), (shards_of,), jnp.float32, low / len(cuts), largest / len(cuts)))
        factor_of = factor_of * jnp.repeat(heights, shape[axis_at] // shards_of).reshape([-1 if axis == axis_at else 1 for axis in range(len(shape))])
    return factor_of


def centred(key, extent, spread, bound, shards=(), kind=jnp.bfloat16):
    result = jax.random.normal(key, extent, jnp.float32) * spread
    if len(shards) > 0:
        result = levels(key, extent, shards, -0.22, 0.18) * result
    return jnp.clip(result, min=-bound, max=bound).astype(kind)


def setup_inputs(seed: int = 0, part: int = 0) -> dict:
    streams_of = jax.random.split(jax.random.key(seed), 9)
    part_splits = jax.random.split(jax.random.fold_in(streams_of[8], part), 9)
    return {
        "tokens": centred(part_splits[0], (TOKENS, D), 1.0, 6.0, ((0, 16),)),
        "routing": draw_routing(jax.random.fold_in(jax.random.fold_in(streams_of[8], part), 71), part),
        "gate_weights": jnp.clip(jnp.exp(math.log(1.0) - 2.9957323 * jax.random.uniform(part_splits[2], (TOKENS, TOPK), jnp.float32) ** levels(part_splits[2], (TOKENS, TOPK), ((0, 16),), -0.2, 0.2)), 0.05, 1.0),
        "pre_gain": jnp.clip(1.0 + 0.18 * jax.random.normal(streams_of[3], (D,), jnp.float32), 0.1, 1.9),
        "w_gate": centred(streams_of[4], (EXPERTS, D, EXPERT_FF), D ** -0.5, 0.125, ((0, 16),)),
        "w_up": centred(streams_of[5], (EXPERTS, D, EXPERT_FF), D ** -0.5, 0.125, ((0, 16),)),
        "w_down": centred(streams_of[6], (EXPERTS, EXPERT_FF, D), EXPERT_FF ** -0.5, 0.25, ((0, 16),)),
        "post_gain": jnp.clip(1.0 + 0.18 * jax.random.normal(streams_of[7], (D,), jnp.float32), 0.1, 1.9),
    }


epsilon = 1e-06

def normalize(values, gain):
    floats = values.astype(jnp.float32)
    return floats * lax.rsqrt(lax.optimization_barrier(jnp.mean(floats * floats, axis=-1, keepdims=True)) + epsilon) * gain

def reference(tokens, routing, gate_weights, pre_gain, w_gate, w_up, w_down, post_gain):
    normed = normalize(tokens, pre_gain).astype(jnp.bfloat16)
    flat_expert = routing.reshape(-1).astype(jnp.int32)
    flat_token = jnp.repeat(jnp.arange(TOKENS, dtype=jnp.int32), TOPK)
    flat_weight = gate_weights.reshape(-1)
    order = jnp.argsort(flat_expert, stable=True)
    sorted_token = flat_token[order]
    sorted_weight = flat_weight[order]
    counts = lax.optimization_barrier(jnp.sum((flat_expert[None, :] == jnp.arange(EXPERTS, dtype=jnp.int32)[:, None]).astype(jnp.int32), axis=1))
    starts = (jnp.cumsum(counts) - counts).astype(jnp.int32)
    most = CAP * N_EP
    token_pad = jnp.concatenate([sorted_token, jnp.full((most,), TOKENS, jnp.int32)])
    weight_pad = jnp.concatenate([sorted_weight, jnp.zeros((most,), jnp.float32)])
    normed_pad = jnp.concatenate([normed, jnp.zeros((1, D), normed.dtype)], axis=0)

    def one_expert(carry, expert):
        begin = starts[expert].astype(jnp.int32)
        index_rows = lax.dynamic_slice(token_pad, (begin,), (most,))
        weight_rows = lax.dynamic_slice(weight_pad, (begin,), (most,))
        live = jnp.arange(most) < counts[expert]
        index_rows = jnp.where(live, index_rows, TOKENS).astype(jnp.int32)
        weight_rows = jnp.where(live, weight_rows, 0.0)
        rows = normed_pad[index_rows]
        gate = jnp.dot(rows, w_gate[expert], preferred_element_type=jnp.float32)
        upward = jnp.dot(rows, w_up[expert], preferred_element_type=jnp.float32)
        hidden = (jax.nn.silu(gate) * upward).astype(jnp.bfloat16)
        output = jnp.dot(hidden, w_down[expert], preferred_element_type=jnp.float32).astype(jnp.bfloat16)
        carry = carry.at[index_rows].add(output.astype(jnp.float32) * weight_rows[:, None])
        return (carry, None)
    start_sum = jnp.zeros((TOKENS + 1, D), jnp.float32)
    mixture = lax.scan(one_expert, start_sum, jnp.arange(EXPERTS, dtype=jnp.int32))[0][:TOKENS]
    return normalize(mixture, post_gain).astype(jnp.bfloat16)
```

```python
import functools

import jax
import jax.numpy as jnp
from jax import lax
from jax.experimental import pallas as pl
from jax.experimental.pallas import tpu as pltpu
from jax.sharding import PartitionSpec as P

epsilon = 1e-06
MESH = pl.DeviceIdType.MESH


def kernel(
    n, tok, rout, gates, pre, wg_hbm, wu_hbm, wd_hbm, post, out,
    gath, part, rcore, ysend, ryy, zsend, rzz, acc, wg, wu, wd,
    ag_send, ag_recv, rs_core_s, rs_core_r, rs_y_s, rs_y_r, rs_z_s, rs_z_r, wsem,
):
    f32, bf16 = jnp.float32, jnp.bfloat16
    rows, width = tok.shape
    zs = n // 4
    me = lax.axis_index("ep")
    z, y, c = me // 4, (me // 2) % 2, me % 2

    def zx(d):
        value, bit = 0, 1
        while bit < zs:
            value = value + ((z // bit + (d // bit) % 2) % 2) * bit
            bit *= 2
        return value

    def dev(zz, yy, cc):
        return (zz * 2 + yy) * 2 + cc

    core_peer = dev(z, y, 1 - c)
    y_peer = dev(z, 1 - y, c)
    z_peer = [None] + [dev(zx(d), y, c) for d in range(1, zs)]

    loads = [
        pltpu.make_async_copy(src.at[0], dst, wsem.at[i])
        for i, (src, dst) in enumerate(((wg_hbm, wg), (wu_hbm, wu), (wd_hbm, wd)))
    ]
    for load in loads:
        load.start()

    barrier = pltpu.get_barrier_semaphore()
    for peer in [core_peer, y_peer] + z_peer[1:]:
        pl.semaphore_signal(barrier, inc=1, device_id={"ep": peer}, device_id_type=MESH)

    values = tok[...].astype(f32)
    scale = lax.rsqrt(jnp.mean(values * values, axis=-1, keepdims=True) + epsilon)
    gath[me, :, :width] = (values * scale * pre[...]).astype(bf16)
    extra = gath.shape[2] - width
    lane = lax.broadcasted_iota(jnp.int32, (rows, extra), 1)
    expert_of = jnp.where(lane < n, lane, lane - n)
    dense = jnp.zeros((rows, extra), f32)
    for k in range(rout.shape[1]):
        dense = dense + jnp.where(expert_of == rout[:, k : k + 1], gates[:, k : k + 1], 0.0)
    high = dense.astype(bf16).astype(f32)
    gath[me, :, width:] = jnp.where(lane < n, high, dense - high).astype(bf16)

    pl.semaphore_wait(barrier, zs + 1)

    def remote(src, dst, ssem, rsem, peer):
        return pltpu.make_async_remote_copy(
            src_ref=src, dst_ref=dst, send_sem=ssem, recv_sem=rsem,
            device_id={"ep": peer}, device_id_type=MESH,
        )

    started = []

    def go(copy):
        copy.start()
        started.append(copy)

    def slot(d, oy, oc):
        return dev(zx(d), y + oy - 2 * y * oy, c + oc - 2 * c * oc)

    def gcopy(d, oy, oc, i, peer):
        ref = gath.at[slot(d, oy, oc)]
        return remote(ref, ref, ag_send.at[i], ag_recv.at[i], peer)

    def gname(d, oy, oc):
        return (d * 2 + oy) * 2 + oc

    def gwait(d, oy, oc):
        gcopy(d, oy, oc, gname(d, oy, oc), core_peer).wait_recv()

    def forward_own(d):
        gwait(d, 0, 0)
        go(gcopy(d, 0, 0, gname(d, 1, 0), y_peer))
        go(gcopy(d, 0, 0, gname(d, 0, 1), core_peer))

    def forward_other(d):
        gwait(d, 1, 0)
        go(gcopy(d, 1, 0, gname(d, 1, 1), core_peer))

    def ffn(d):
        gwait(d, 0, 1)
        gwait(d, 1, 1)
        base = zx(d) * 4
        x = gath[pl.ds(base, 4), :, :width].reshape(4 * rows, width)
        gate = jnp.dot(x, wg[...], preferred_element_type=f32)
        up = jnp.dot(x, wu[...], preferred_element_type=f32)
        hidden = (gate / (1.0 + jnp.exp(-gate)) * up).astype(bf16)
        ext = gath[pl.ds(base, 4), :, width:].reshape(4 * rows, extra).astype(f32)
        lanes = lax.broadcasted_iota(jnp.int32, ext.shape, 1)
        mine = (lanes == me) | (lanes == me + n)
        weight = jnp.sum(jnp.where(mine, ext, 0.0), axis=-1, keepdims=True)
        served = jnp.dot(hidden, wd[...], preferred_element_type=f32) * weight
        part[d] = served.astype(bf16).reshape(4, rows, width)

    def core_copy(d, yy, cc):
        i = d * 2 + yy
        return remote(
            part.at[d, yy * 2 + cc], rcore.at[d, yy], rs_core_s.at[i], rs_core_r.at[i], core_peer
        )

    def send_core(d):
        for yy in range(2):
            go(core_copy(d, yy, 1 - c))

    def y_copy(d):
        return remote(ysend.at[d], ryy.at[d], rs_y_s.at[d], rs_y_r.at[d], y_peer)

    def send_y(d):
        for yy in range(2):
            core_copy(d, yy, 1 - c).wait_recv()
        oy = 1 - y
        ysend[d] = (part[d, oy * 2 + c].astype(f32) + rcore[d, oy].astype(f32)).astype(bf16)
        go(y_copy(d))

    def z_copy(d):
        return remote(zsend.at[d], rzz.at[d], rs_z_s.at[d], rs_z_r.at[d], z_peer[d])

    def send_z(d):
        y_copy(d).wait_recv()
        total = part[d, y * 2 + c].astype(f32) + rcore[d, y].astype(f32) + ryy[d].astype(f32)
        if d == 0:
            acc[...] = total
        else:
            zsend[d] = total.astype(bf16)
            go(z_copy(d))

    own = gath.at[me]
    go(remote(own, own, ag_send.at[gname(0, 1, 0)], ag_recv.at[gname(0, 1, 0)], y_peer))
    go(remote(own, own, ag_send.at[gname(0, 0, 1)], ag_recv.at[gname(0, 0, 1)], core_peer))
    for d in range(1, zs):
        i = gname(d, 0, 0)
        go(remote(own, own, ag_send.at[i], ag_recv.at[i], z_peer[d]))

    if zs > 1:
        forward_own(1)
    forward_other(0)
    for load in loads:
        load.wait()
    for d in range(zs):
        ffn(d)
        send_core(d)
        if d + 2 < zs:
            forward_own(d + 2)
        if d + 1 < zs:
            forward_other(d + 1)
        send_y(d)
        if d > 0:
            send_z(d - 1)
    send_z(zs - 1)
    total = acc[...]
    for d in range(1, zs):
        z_copy(d).wait_recv()
        total = total + rzz[d].astype(f32)
    scale = lax.rsqrt(jnp.mean(total * total, axis=-1, keepdims=True) + epsilon)
    out[...] = (total * scale * post[...]).astype(out.dtype)
    for copy in started:
        copy.wait_send()


def body(tokens, routing, gate_weights, pre_gain, w_gate, w_up, w_down, post_gain):
    n = lax.axis_size("ep")
    rows, width = tokens.shape
    ff = w_gate.shape[2]
    zs = n // 4
    extra = -(-2 * n // 128) * 128
    bf16, dma = jnp.bfloat16, pltpu.SemaphoreType.DMA
    vmem = pl.BlockSpec(memory_space=pltpu.VMEM)
    hbm = pl.BlockSpec(memory_space=pl.ANY)
    return pl.pallas_call(
        functools.partial(kernel, n),
        out_shape=jax.ShapeDtypeStruct((rows, width), bf16),
        in_specs=[vmem, vmem, vmem, vmem, hbm, hbm, hbm, vmem],
        out_specs=vmem,
        scratch_shapes=[
            pltpu.VMEM((n, rows, width + extra), bf16),
            pltpu.VMEM((zs, 4, rows, width), bf16),
            pltpu.VMEM((zs, 2, rows, width), bf16),
            pltpu.VMEM((zs, rows, width), bf16),
            pltpu.VMEM((zs, rows, width), bf16),
            pltpu.VMEM((zs, rows, width), bf16),
            pltpu.VMEM((zs, rows, width), bf16),
            pltpu.VMEM((rows, width), jnp.float32),
            pltpu.VMEM((width, ff), bf16),
            pltpu.VMEM((width, ff), bf16),
            pltpu.VMEM((ff, width), bf16),
            dma((n,)), dma((n,)),
            dma((2 * zs,)), dma((2 * zs,)),
            dma((zs,)), dma((zs,)), dma((zs,)), dma((zs,)),
            dma((3,)),
        ],
        compiler_params=pltpu.CompilerParams(
            collective_id=0, has_side_effects=True, vmem_limit_bytes=60 * 1024 * 1024
        ),
    )(
        tokens, routing, gate_weights, pre_gain.reshape(1, width),
        w_gate, w_up, w_down, post_gain.reshape(1, width),
    )


def solution(mesh):
    rows = P(("grp", "ep"), None)
    expert = P("ep", None, None)
    in_specs = (rows, rows, rows, P(), expert, expert, expert, P())
    return jax.shard_map(body, mesh=mesh, in_specs=in_specs, out_specs=rows, check_vma=False)
```

```python
import functools

import jax
import jax.numpy as jnp
from jax import lax
from jax.experimental import pallas as pl
from jax.experimental.pallas import tpu as pltpu
from jax.sharding import PartitionSpec as P

epsilon = 1e-06
MESH = pl.DeviceIdType.MESH


def kernel(
    n, parts, tok, rout, gates, pre, wg_hbm, wu_hbm, wd_hbm, post, out,
    gath, part, rcore, ysend, ryy, zsend, rzz, acc, wg, wu, wd,
    ag_send, ag_recv, rs_core_s, rs_core_r, rs_y_s, rs_y_r, rs_z_s, rs_z_r, wsem,
):
    f32, bf16 = jnp.float32, jnp.bfloat16
    rows, width = tok.shape
    zs = n // 4
    me = lax.axis_index("ep")
    z, y, c = me // 4, (me // 2) % 2, me % 2

    def zx(d):
        value, bit = 0, 1
        while bit < zs:
            value = value + ((z // bit + (d // bit) % 2) % 2) * bit
            bit *= 2
        return value

    def dev(zz, yy, cc):
        return (zz * 2 + yy) * 2 + cc

    core_peer = dev(z, y, 1 - c)
    y_peer = dev(z, 1 - y, c)
    z_peer = [None] + [dev(zx(d), y, c) for d in range(1, zs)]

    loads = [
        pltpu.make_async_copy(src.at[0], dst, wsem.at[i])
        for i, (src, dst) in enumerate(((wg_hbm, wg), (wu_hbm, wu), (wd_hbm, wd)))
    ]
    for load in loads:
        load.start()

    barrier = pltpu.get_barrier_semaphore()
    for peer in [core_peer, y_peer] + z_peer[1:]:
        pl.semaphore_signal(barrier, inc=1, device_id={"ep": peer}, device_id_type=MESH)

    values = tok[...].astype(f32)
    scale = lax.rsqrt(jnp.mean(values * values, axis=-1, keepdims=True) + epsilon)
    normed = (values * scale * pre[...]).astype(bf16)
    extra = gath.shape[3] - width
    sub = lax.broadcasted_iota(jnp.int32, (extra, rows), 0)
    expert_of = jnp.where(sub < n, sub, sub - n)
    dense = jnp.zeros((extra, rows), f32)
    for k in range(rout.shape[0]):
        dense = dense + jnp.where(expert_of == rout[k : k + 1, :], gates[k : k + 1, :], 0.0)
    high = dense.astype(bf16).astype(f32)
    mixing = jnp.where(sub < n, high, dense - high).T.astype(bf16)
    piece = rows // parts
    for h in range(parts):
        gath[h, me, :, :width] = normed[h * piece : (h + 1) * piece]
        gath[h, me, :, width:] = mixing[h * piece : (h + 1) * piece]

    pl.semaphore_wait(barrier, zs + 1)

    def remote(src, dst, ssem, rsem, peer):
        return pltpu.make_async_remote_copy(
            src_ref=src, dst_ref=dst, send_sem=ssem, recv_sem=rsem,
            device_id={"ep": peer}, device_id_type=MESH,
        )

    started = []

    def go(copy):
        copy.start()
        started.append(copy)

    def slot(d, h, oy, oc):
        return gath.at[h, dev(zx(d), y + oy - 2 * y * oy, c + oc - 2 * c * oc)]

    def gname(d, h, oy, oc):
        return ((d * parts + h) * 2 + oy) * 2 + oc

    def gcopy(d, h, oy, oc, i, peer):
        ref = slot(d, h, oy, oc)
        return remote(ref, ref, ag_send.at[i], ag_recv.at[i], peer)

    def gwait(d, h, oy, oc):
        gcopy(d, h, oy, oc, gname(d, h, oy, oc), core_peer).wait_recv()

    def forward_own(d, h):
        if d > 0:
            gwait(d, h, 0, 0)
            go(gcopy(d, h, 0, 0, gname(d, h, 1, 0), y_peer))
            go(gcopy(d, h, 0, 0, gname(d, h, 0, 1), core_peer))

    def forward_other(d, h):
        gwait(d, h, 1, 0)
        go(gcopy(d, h, 1, 0, gname(d, h, 1, 1), core_peer))

    def at(d, h):
        return d * parts + h

    def core_copy(d, h, yy):
        i = at(d, h) * 2 + yy
        return remote(
            part.at[at(d, h), yy * 2 + 1 - c], rcore.at[at(d, h), yy],
            rs_core_s.at[i], rs_core_r.at[i], core_peer,
        )

    def ffn(d, h):
        gwait(d, h, 0, 1)
        gwait(d, h, 1, 1)
        base = zx(d) * 4
        x = gath[h, pl.ds(base, 4), :, :width].reshape(4 * piece, width)
        gate = jnp.dot(x, wg[...], preferred_element_type=f32)
        up = jnp.dot(x, wu[...], preferred_element_type=f32)
        hidden = (gate / (1.0 + jnp.exp(-gate)) * up).astype(bf16)
        ext = gath[h, pl.ds(base, 4), :, width:].reshape(4 * piece, extra).astype(f32)
        lanes = lax.broadcasted_iota(jnp.int32, ext.shape, 1)
        mine = (lanes == me) | (lanes == me + n)
        weight = jnp.sum(jnp.where(mine, ext, 0.0), axis=-1, keepdims=True)
        served = jnp.dot(hidden, wd[...], preferred_element_type=f32) * weight
        part[at(d, h)] = served.astype(bf16).reshape(4, piece, width)
        for yy in range(2):
            go(core_copy(d, h, yy))

    def y_copy(d, h):
        i = at(d, h)
        return remote(ysend.at[i], ryy.at[i], rs_y_s.at[i], rs_y_r.at[i], y_peer)

    def send_y(d, h):
        for yy in range(2):
            core_copy(d, h, yy).wait_recv()
        i, oy = at(d, h), 1 - y
        ysend[i] = (part[i, oy * 2 + c].astype(f32) + rcore[i, oy].astype(f32)).astype(bf16)
        go(y_copy(d, h))

    def z_copy(d, h):
        i = at(d, h)
        return remote(zsend.at[i], rzz.at[i], rs_z_s.at[i], rs_z_r.at[i], z_peer[d])

    def send_z(d, h):
        y_copy(d, h).wait_recv()
        i = at(d, h)
        total = part[i, y * 2 + c].astype(f32) + rcore[i, y].astype(f32) + ryy[i].astype(f32)
        if d == 0:
            acc[h] = total
        else:
            zsend[i] = total.astype(bf16)
            go(z_copy(d, h))

    order = ([0, 1] + list(range(2, zs))[::-1])[:zs]
    steps = [(d, h) for d in order for h in range(parts)]

    for h in range(parts):
        own = gath.at[h, me]
        for d, oy, oc, peer in ((0, 1, 0, y_peer), (0, 0, 1, core_peer)):
            i = gname(d, h, oy, oc)
            go(remote(own, own, ag_send.at[i], ag_recv.at[i], peer))
    for d, h in steps:
        if d > 0:
            i = gname(d, h, 0, 0)
            own = gath.at[h, me]
            go(remote(own, own, ag_send.at[i], ag_recv.at[i], z_peer[d]))
    for load in loads:
        load.wait()

    events = []
    for i, step in enumerate(steps):
        for lag, event in ((0, forward_own), (4, forward_other), (5.5, ffn), (8, send_y), (12.5, send_z)):
            events.append((4 * i / parts + lag, len(events), event, step))
    for _, _, event, step in sorted(events, key=lambda e: e[:2]):
        event(*step)

    for h in range(parts):
        total = acc[h]
        for d in order[1:]:
            z_copy(d, h).wait_recv()
            total = total + rzz[at(d, h)].astype(f32)
        scale = lax.rsqrt(jnp.mean(total * total, axis=-1, keepdims=True) + epsilon)
        out[h * piece : (h + 1) * piece, :] = (total * scale * post[...]).astype(out.dtype)
    for copy in started:
        copy.wait_send()


def body(tokens, routing, gate_weights, pre_gain, w_gate, w_up, w_down, post_gain):
    n = lax.axis_size("ep")
    rows, width = tokens.shape
    ff = w_gate.shape[2]
    zs = n // 4
    parts = 2 if rows % 32 == 0 and zs <= 4 else 1
    piece, count = rows // parts, zs * parts
    extra = -(-2 * n // 128) * 128
    bf16, dma = jnp.bfloat16, pltpu.SemaphoreType.DMA
    vmem = pl.BlockSpec(memory_space=pltpu.VMEM)
    hbm = pl.BlockSpec(memory_space=pl.ANY)
    return pl.pallas_call(
        functools.partial(kernel, n, parts),
        out_shape=jax.ShapeDtypeStruct((rows, width), bf16),
        in_specs=[vmem, vmem, vmem, vmem, hbm, hbm, hbm, vmem],
        out_specs=vmem,
        scratch_shapes=[
            pltpu.VMEM((parts, n, piece, width + extra), bf16),
            pltpu.VMEM((count, 4, piece, width), bf16),
            pltpu.VMEM((count, 2, piece, width), bf16),
            pltpu.VMEM((count, piece, width), bf16),
            pltpu.VMEM((count, piece, width), bf16),
            pltpu.VMEM((count, piece, width), bf16),
            pltpu.VMEM((count, piece, width), bf16),
            pltpu.VMEM((parts, piece, width), jnp.float32),
            pltpu.VMEM((width, ff), bf16),
            pltpu.VMEM((width, ff), bf16),
            pltpu.VMEM((ff, width), bf16),
            dma((4 * count,)), dma((4 * count,)),
            dma((2 * count,)), dma((2 * count,)),
            dma((count,)), dma((count,)), dma((count,)), dma((count,)),
            dma((3,)),
        ],
        compiler_params=pltpu.CompilerParams(
            collective_id=0, has_side_effects=True, vmem_limit_bytes=60 * 1024 * 1024
        ),
    )(
        tokens, routing.T, gate_weights.T, pre_gain.reshape(1, width),
        w_gate, w_up, w_down, post_gain.reshape(1, width),
    )


def solution(mesh):
    rows = P(("grp", "ep"), None)
    expert = P("ep", None, None)
    in_specs = (rows, rows, rows, P(), expert, expert, expert, P())
    return jax.shard_map(body, mesh=mesh, in_specs=in_specs, out_specs=rows, check_vma=False)
```

```python
import functools

import jax
import jax.numpy as jnp
from jax import lax
from jax.experimental import pallas as pl
from jax.experimental.pallas import tpu as pltpu
from jax.sharding import PartitionSpec as P

epsilon = 1e-06
MESH = pl.DeviceIdType.MESH


def kernel(
    n, parts, tok, rout, gates, pre, wg_hbm, wu_hbm, wd_hbm, post, out,
    gath, part, rcore, ysend, ryy, zsend, rzz, acc, wg, wu, wd,
    ag_send, ag_recv, rs_core_s, rs_core_r, rs_y_s, rs_y_r, rs_z_s, rs_z_r, wsem,
):
    f32, bf16 = jnp.float32, jnp.bfloat16
    rows, width = tok.shape
    zs = n // 4
    me = lax.axis_index("ep")
    z, y, c = me // 4, (me // 2) % 2, me % 2

    def zx(d):
        value, bit = 0, 1
        while bit < zs:
            value = value + ((z // bit + (d // bit) % 2) % 2) * bit
            bit *= 2
        return value

    def dev(zz, yy, cc):
        return (zz * 2 + yy) * 2 + cc

    core_peer = dev(z, y, 1 - c)
    y_peer = dev(z, 1 - y, c)
    z_peer = [None] + [dev(zx(d), y, c) for d in range(1, zs)]

    loads = [
        pltpu.make_async_copy(src.at[0], dst, wsem.at[i])
        for i, (src, dst) in enumerate(((wg_hbm, wg), (wu_hbm, wu), (wd_hbm, wd)))
    ]
    for load in loads:
        load.start()

    barrier = pltpu.get_barrier_semaphore()
    for peer in [core_peer, y_peer] + z_peer[1:]:
        pl.semaphore_signal(barrier, inc=1, device_id={"ep": peer}, device_id_type=MESH)

    values = tok[...].astype(f32)
    scale = lax.rsqrt(jnp.mean(values * values, axis=-1, keepdims=True) + epsilon)
    normed = (values * scale * pre[...]).astype(bf16)
    extra = gath.shape[3] - width
    sub = lax.broadcasted_iota(jnp.int32, (extra, rows), 0)
    expert_of = jnp.where(sub < n, sub, sub - n)
    dense = jnp.zeros((extra, rows), f32)
    for k in range(rout.shape[0]):
        dense = dense + jnp.where(expert_of == rout[k : k + 1, :], gates[k : k + 1, :], 0.0)
    high = dense.astype(bf16).astype(f32)
    mixing = jnp.where(sub < n, high, dense - high).T.astype(bf16)
    piece = rows // parts
    for h in range(parts):
        gath[h, me, :, :width] = normed[h * piece : (h + 1) * piece]
        gath[h, me, :, width:] = mixing[h * piece : (h + 1) * piece]

    pl.semaphore_wait(barrier, zs + 1)

    def remote(src, dst, ssem, rsem, peer):
        return pltpu.make_async_remote_copy(
            src_ref=src, dst_ref=dst, send_sem=ssem, recv_sem=rsem,
            device_id={"ep": peer}, device_id_type=MESH,
        )

    started = []

    def go(copy):
        copy.start()
        started.append(copy)

    def slot(d, h, oy, oc):
        return gath.at[h, dev(zx(d), y + oy - 2 * y * oy, c + oc - 2 * c * oc)]

    def gname(d, h, oy, oc):
        return ((d * parts + h) * 2 + oy) * 2 + oc

    def gcopy(d, h, oy, oc, i, peer):
        ref = slot(d, h, oy, oc)
        return remote(ref, ref, ag_send.at[i], ag_recv.at[i], peer)

    def gwait(d, h, oy, oc):
        gcopy(d, h, oy, oc, gname(d, h, oy, oc), core_peer).wait_recv()

    def forward_own(d, h):
        if d > 0:
            gwait(d, h, 0, 0)
            go(gcopy(d, h, 0, 0, gname(d, h, 1, 0), y_peer))
            go(gcopy(d, h, 0, 0, gname(d, h, 0, 1), core_peer))

    def forward_other(d, h):
        gwait(d, h, 1, 0)
        go(gcopy(d, h, 1, 0, gname(d, h, 1, 1), core_peer))

    def at(d, h):
        return d * parts + h

    def core_copy(d, h, yy):
        i = at(d, h) * 2 + yy
        return remote(
            part.at[at(d, h), yy * 2 + 1 - c], rcore.at[at(d, h), yy],
            rs_core_s.at[i], rs_core_r.at[i], core_peer,
        )

    def ffn(d, h):
        gwait(d, h, 0, 1)
        gwait(d, h, 1, 1)
        base = zx(d) * 4
        x = gath[h, pl.ds(base, 4), :, :width].reshape(4 * piece, width)
        gate = jnp.dot(x, wg[...], preferred_element_type=f32)
        up = jnp.dot(x, wu[...], preferred_element_type=f32)
        hidden = (gate / (1.0 + jnp.exp(-gate)) * up).astype(bf16)
        ext = gath[h, pl.ds(base, 4), :, width:].reshape(4 * piece, extra).astype(f32)
        lanes = lax.broadcasted_iota(jnp.int32, ext.shape, 1)
        mine = (lanes == me) | (lanes == me + n)
        weight = jnp.sum(jnp.where(mine, ext, 0.0), axis=-1, keepdims=True)
        served = jnp.dot(hidden, wd[...], preferred_element_type=f32) * weight
        part[at(d, h)] = served.astype(bf16).reshape(4, piece, width)
        for yy in range(2):
            go(core_copy(d, h, yy))

    def y_copy(d, h):
        i = at(d, h)
        return remote(ysend.at[i], ryy.at[i], rs_y_s.at[i], rs_y_r.at[i], y_peer)

    def send_y(d, h):
        for yy in range(2):
            core_copy(d, h, yy).wait_recv()
        i, oy = at(d, h), 1 - y
        ysend[i] = (part[i, oy * 2 + c].astype(f32) + rcore[i, oy].astype(f32)).astype(bf16)
        go(y_copy(d, h))

    def z_copy(d, h):
        i = at(d, h)
        return remote(zsend.at[i], rzz.at[i], rs_z_s.at[i], rs_z_r.at[i], z_peer[d])

    def send_z(d, h):
        y_copy(d, h).wait_recv()
        i = at(d, h)
        total = part[i, y * 2 + c].astype(f32) + rcore[i, y].astype(f32) + ryy[i].astype(f32)
        if d == 0:
            acc[h] = total
        else:
            zsend[i] = total.astype(bf16)
            go(z_copy(d, h))

    order = list(range(zs))
    steps = [(d, h) for d in order for h in range(parts)]

    for h in range(parts):
        own = gath.at[h, me]
        for d, oy, oc, peer in ((0, 1, 0, y_peer), (0, 0, 1, core_peer)):
            i = gname(d, h, oy, oc)
            go(remote(own, own, ag_send.at[i], ag_recv.at[i], peer))
    for d, h in steps:
        if d > 0:
            i = gname(d, h, 0, 0)
            own = gath.at[h, me]
            go(remote(own, own, ag_send.at[i], ag_recv.at[i], z_peer[d]))
    for load in loads:
        load.wait()

    events = []
    for i, step in enumerate(steps):
        for lag, event in ((0, forward_own), (4, forward_other), (5.5, ffn), (8, send_y), (12.5, send_z)):
            events.append((4 * i / parts + lag, len(events), event, step))
    for _, _, event, step in sorted(events, key=lambda e: e[:2]):
        event(*step)

    for h in range(parts):
        total = acc[h]
        for d in order[1:]:
            z_copy(d, h).wait_recv()
            total = total + rzz[at(d, h)].astype(f32)
        scale = lax.rsqrt(jnp.mean(total * total, axis=-1, keepdims=True) + epsilon)
        out[h * piece : (h + 1) * piece, :] = (total * scale * post[...]).astype(out.dtype)
    for copy in started:
        copy.wait_send()


def body(tokens, routing, gate_weights, pre_gain, w_gate, w_up, w_down, post_gain):
    n = lax.axis_size("ep")
    rows, width = tokens.shape
    ff = w_gate.shape[2]
    zs = n // 4
    parts = 1
    piece, count = rows // parts, zs * parts
    extra = -(-2 * n // 128) * 128
    bf16, dma = jnp.bfloat16, pltpu.SemaphoreType.DMA
    vmem = pl.BlockSpec(memory_space=pltpu.VMEM)
    hbm = pl.BlockSpec(memory_space=pl.ANY)
    return pl.pallas_call(
        functools.partial(kernel, n, parts),
        out_shape=jax.ShapeDtypeStruct((rows, width), bf16),
        in_specs=[vmem, vmem, vmem, vmem, hbm, hbm, hbm, vmem],
        out_specs=vmem,
        scratch_shapes=[
            pltpu.VMEM((parts, n, piece, width + extra), bf16),
            pltpu.VMEM((count, 4, piece, width), bf16),
            pltpu.VMEM((count, 2, piece, width), bf16),
            pltpu.VMEM((count, piece, width), bf16),
            pltpu.VMEM((count, piece, width), bf16),
            pltpu.VMEM((count, piece, width), bf16),
            pltpu.VMEM((count, piece, width), bf16),
            pltpu.VMEM((parts, piece, width), jnp.float32),
            pltpu.VMEM((width, ff), bf16),
            pltpu.VMEM((width, ff), bf16),
            pltpu.VMEM((ff, width), bf16),
            dma((4 * count,)), dma((4 * count,)),
            dma((2 * count,)), dma((2 * count,)),
            dma((count,)), dma((count,)), dma((count,)), dma((count,)),
            dma((3,)),
        ],
        compiler_params=pltpu.CompilerParams(
            collective_id=0, has_side_effects=True, vmem_limit_bytes=60 * 1024 * 1024
        ),
    )(
        tokens, routing.T, gate_weights.T, pre_gain.reshape(1, width),
        w_gate, w_up, w_down, post_gain.reshape(1, width),
    )


def solution(mesh):
    rows = P(("grp", "ep"), None)
    expert = P("ep", None, None)
    in_specs = (rows, rows, rows, P(), expert, expert, expert, P())
    return jax.shard_map(body, mesh=mesh, in_specs=in_specs, out_specs=rows, check_vma=False)
```
